32 devices in a mesh: sp: 8 (over z, x), tp: 4 (over y, core).
Axes of the slice: x: 2, y: 2, z: 4, core: 2. Of those that a mesh axis runs over, the one named last changes fastest.
Arguments:
- residual: bfloat16 [3072, 2048], P('sp', 'tp'), may hold values from -6 to 6
- query_nope: bfloat16 [3072, 4096], P('sp', 'tp'), may hold values from -9 to 9
- query_rope: bfloat16 [3072, 2048], P('sp', 'tp'), may hold values from -600 to 600
- latent: bfloat16 [3072, 512], P('sp'), may hold values from -6 to 6
- rope_key: bfloat16 [3072, 64], P('sp'), may hold values from -6 to 6
- doc_ids: int32 [3072], P('sp'), may hold values from 0 to 3, never falling along the last dimension, each value on 1 to 1152 neighbouring positions
- key_up: bfloat16 [512, 4096], P(None, 'tp'), may hold values from -0.25 to 0.25
- value_up: bfloat16 [512, 4096], P(None, 'tp'), may hold values from -0.25 to 0.25
- out_proj: bfloat16 [4096, 2048], P('tp'), may hold values from -0.375 to 0.375
- norm1_gain: bfloat16 [2048], P('tp'), may hold values from 0.099609375 to 1.8984375
- norm1_bias: bfloat16 [2048], P('tp'), may hold values from -3 to 3
- ffn_gate: bfloat16 [2048, 5632], P('sp', 'tp'), may hold values from -0.125 to 0.125
- ffn_value: bfloat16 [2048, 5632], P('sp', 'tp'), may hold values from -0.125 to 0.125
- conv_gate: bfloat16 [3, 5632], P(None, 'tp'), may hold values from -3.5 to 3.5
- conv_value: bfloat16 [3, 5632], P(None, 'tp'), may hold values from -3.5 to 3.5
- ffn_down: bfloat16 [5632, 2048], P('tp', 'sp'), may hold values from -0.15625 to 0.15625
- norm2_gain: bfloat16 [2048], P('tp'), may hold values from 0.099609375 to 1.8984375
- norm2_bias: bfloat16 [2048], P('tp'), may hold values from -3 to 3
Outputs:
- layer_out: bfloat16 [3072, 2048], P('sp', 'tp')
The draws below stay inside these ranges and needn't reach their ends.
Inputs may be any that keep to these rules, and one draw needn't show every extreme that they name: `doc_ids`: document numbers never fall along the positions; each document holds 1 to 1152 positions, and one holds exactly 1152.
All inputs are finite; a program needn't handle non-finite values.
Results may differ from the reference program's by a relative error of at most 0.014.
Values may be sent and summed in bfloat16 or wider, within the bound.
A program may use at most 128 MiB of HBM per device.

```python
import math
import jax
import jax.numpy as jnp
import numpy as np
from jax import lax

D = 2048
HEADS = 32
NOPE = 128
ROPE = 64
VDIM = 128
LATENT = 512
FF = 5632
CONV = 3
REACH = 3
TOK_DEV = 384
TOKENS = 3072
DOCS = 4
N_SP = 8
N_TP = 4


def rope_base(key):
    base_rows = jnp.clip(jax.random.normal(jax.random.fold_in(key, 7), (TOKENS, ROPE), jnp.float32), -6.0, 6.0)
    return base_rows


def draw_rope_key(key, part):
    return rope_base(key).astype(jnp.bfloat16)


def draw_query_rope(key, part):
    drawn = jnp.clip(jax.random.normal(jax.random.fold_in(key, 9), (TOKENS, HEADS * ROPE), jnp.float32), -6.0, 6.0) * 1.5
    return drawn.astype(jnp.bfloat16)


def shard_levels(own_key, extent, cuts, low, largest):
    gain = 1.0
    for dim, shards_of in cuts:
        draws = jax.random.uniform(jax.random.fold_in(jax.random.fold_in(own_key, 6), dim), (shards_of,), jnp.float32, low / len(cuts), largest / len(cuts))
        gain = gain * jnp.repeat(jnp.exp(draws), extent[dim] // shards_of).reshape((-1,) + (1,) * (len(extent) - 1 - dim))
    return gain


def profile(number_of, total, most, lean):
    loads = [(1 << 20) // math.isqrt(rank ** lean) + 1 for rank in range(2, number_of + 1)]
    spare, counts = total - most - (number_of - 1), [1] * (number_of - 1)
    while spare > 0:
        candidates = [i for i in range(number_of - 1) if counts[i] < most]
        whole, remaining = sum([loads[i] for i in candidates]), spare
        for i in candidates:
            extra = min(most - counts[i], max(1, remaining * loads[i] // whole), spare)
            counts[i] = counts[i] + extra
            spare = spare - extra
    return np.array([most] + counts)


def ragged_sizes(own_key, count, total, most, skew):
    if count == 2:
        one = jax.random.randint(own_key, (), max(1, total - most), min(most, total - 1) + 1)
        return jnp.stack([one, total - one])
    lengths = jnp.asarray(profile(count, total, most, skew), jnp.int32)
    pairs = (count - 1) // 2
    donor, sink = lengths[1:1 + 2 * pairs:2], lengths[2:2 + 2 * pairs:2]
    room = jnp.minimum(donor - 1, most - sink)
    shifted = jax.random.randint(jax.random.fold_in(own_key, 1), (pairs,), 0, 1 << 20) % (room + 1)
    lengths = lengths.at[1:1 + 2 * pairs:2].set(donor - shifted).at[2:2 + 2 * pairs:2].set(sink + shifted)
    return lengths[jax.random.permutation(jax.random.fold_in(own_key, 2), count)]


def noise(own_key, dims, scale, bound, split=(), kind=jnp.bfloat16):
    gain = shard_levels(own_key, dims, split, -0.22, 0.18) if split else 1.0
    values = jax.random.normal(own_key, dims, jnp.float32) * scale * gain
    return jnp.minimum(jnp.maximum(values, -bound), bound).astype(kind)


def setup_inputs(seed: int = 0) -> dict:
    key_of = jax.random.split(jax.random.key(seed), 19)
    residual = noise(key_of[0], (TOKENS, D), 1.0, 6.0, ((0, 8), (1, 4)))
    query_nope = noise(key_of[1], (TOKENS, HEADS * NOPE), 1.5, 9.0, ((0, 8), (1, 4)))
    query_rope = draw_query_rope(jax.random.fold_in(key_of[18], 71), 0)
    latent = noise(key_of[3], (TOKENS, LATENT), 1.0, 6.0, ((0, 8),))
    rope_key = draw_rope_key(jax.random.fold_in(key_of[18], 71), 0)
    doc_ids = jnp.searchsorted(jnp.cumsum(ragged_sizes(key_of[5], DOCS, TOKENS, REACH * TOK_DEV, 1)), jnp.arange(TOKENS), side="right").astype(jnp.int32)
    key_up = noise(key_of[6], (LATENT, HEADS * NOPE), LATENT ** -0.5, 0.25, ((1, 4),))
    value_up = noise(key_of[7], (LATENT, HEADS * VDIM), LATENT ** -0.5, 0.25, ((1, 4),))
    out_proj = noise(key_of[8], (HEADS * VDIM, D), (HEADS * VDIM // 16) ** -0.5, 0.375, ((0, 4),))
    norm1_gain = jnp.clip(1.0 + 0.18 * jax.random.normal(key_of[9], (D,), jnp.float32), 0.099609375, 1.8984375).astype(jnp.bfloat16)
    norm1_bias = noise(key_of[10], (D,), 0.5, 3.0, ((0, 4),))
    ffn_gate = noise(key_of[11], (D, FF), D ** -0.5, 0.125, ((0, 8), (1, 4)))
    ffn_value = noise(key_of[12], (D, FF), D ** -0.5, 0.125, ((0, 8), (1, 4)))
    conv_gate = noise(key_of[13], (CONV, FF), CONV ** -0.5, 3.5, ((1, 4),))
    conv_value = noise(key_of[14], (CONV, FF), CONV ** -0.5, 3.5, ((1, 4),))
    ffn_down = noise(key_of[15], (FF, D), (FF // 4) ** -0.5, 0.15625, ((0, 4), (1, 8)))
    norm2_gain = jnp.clip(1.0 + 0.18 * jax.random.normal(key_of[16], (D,), jnp.float32), 0.099609375, 1.8984375).astype(jnp.bfloat16)
    norm2_bias = noise(key_of[17], (D,), 0.5, 3.0, ((0, 4),))
    return dict(residual=residual, query_nope=query_nope, query_rope=query_rope, latent=latent, rope_key=rope_key, doc_ids=doc_ids, key_up=key_up, value_up=value_up, out_proj=out_proj, norm1_gain=norm1_gain, norm1_bias=norm1_bias, ffn_gate=ffn_gate, ffn_value=ffn_value, conv_gate=conv_gate, conv_value=conv_value, ffn_down=ffn_down, norm2_gain=norm2_gain, norm2_bias=norm2_bias)


norm_eps = 1e-05
residual_scale = 8.0 ** 0.25
rope_base_freq = 10000.0
masked_score = -1e+30

def tables(positions):
    frequencies = 1.0 / rope_base_freq ** (jnp.arange(0, ROPE, 2, dtype=jnp.float32) / ROPE)
    angles = positions.astype(jnp.float32)[:, None] * frequencies[None, :]
    return (jnp.cos(angles), jnp.sin(angles))

def rotate(vectors, cosine, sine_table):
    half_width = vectors.shape[-1] // 2
    front_half = vectors[..., :half_width]
    back_half = vectors[..., half_width:]
    return jnp.concatenate([front_half * cosine - back_half * sine_table, front_half * sine_table + back_half * cosine], axis=-1)

def layer_norm(mixed, gain_row, bias_row):
    width = mixed.shape[-1]
    row_mean = lax.optimization_barrier(jnp.sum(mixed, -1, keepdims=True)) / width
    row_power = lax.optimization_barrier(jnp.sum(mixed * mixed, -1, keepdims=True)) / width
    return (mixed - row_mean) * lax.rsqrt(row_power - row_mean * row_mean + norm_eps) * gain_row.astype(jnp.float32) + bias_row.astype(jnp.float32)

def reference(residual, query_nope, query_rope, latent, rope_key, doc_ids, key_up, value_up, out_proj, norm1_gain, norm1_bias, ffn_gate, ffn_value, conv_gate, conv_value, ffn_down, norm2_gain, norm2_bias):
    row_count = TOK_DEV
    window = (REACH + 1) * row_count
    lead_rows = REACH * row_count
    rim_rows = CONV - 1
    positions = jnp.arange(TOKENS, dtype=jnp.int32)
    cosine, sine_table = tables(positions)
    turned_key = rotate(rope_key.astype(jnp.float32), cosine, sine_table).astype(jnp.bfloat16)
    turned_query = rotate(query_rope.astype(jnp.float32).reshape(TOKENS, HEADS, ROPE), cosine[:, None], sine_table[:, None]).astype(jnp.bfloat16)
    padded_latent = jnp.concatenate([jnp.zeros((lead_rows, LATENT), jnp.bfloat16), latent], 0)
    padded_key = jnp.concatenate([jnp.zeros((lead_rows, ROPE), jnp.bfloat16), turned_key], 0)
    padded_doc = jnp.concatenate([jnp.full((lead_rows,), -1, jnp.int32), doc_ids], 0)
    head_group = HEADS * VDIM // N_TP
    scale = (NOPE + ROPE) ** (-0.5)

    def first_half(block_index):
        row_start = (block_index * row_count).astype(jnp.int32)
        own_pos = row_start + jnp.arange(row_count, dtype=jnp.int32)
        win_latent = lax.dynamic_slice_in_dim(padded_latent, row_start, window, 0)
        win_key = lax.dynamic_slice_in_dim(padded_key, row_start, window, 0)
        win_doc = lax.dynamic_slice_in_dim(padded_doc, row_start, window, 0)
        own_doc = lax.dynamic_slice_in_dim(doc_ids, row_start, row_count, 0)
        key_pos = row_start - lead_rows + jnp.arange(window, dtype=jnp.int32)
        allowed = (key_pos[None, :] <= own_pos[:, None]) & (key_pos[None, :] >= 0) & (win_doc[None, :] == own_doc[:, None])
        key_rows = jnp.dot(win_latent, key_up, preferred_element_type=jnp.float32).astype(jnp.bfloat16).reshape(window, HEADS, NOPE)
        values = jnp.dot(win_latent, value_up, preferred_element_type=jnp.float32).astype(jnp.bfloat16).reshape(window, HEADS, VDIM)
        queries = lax.dynamic_slice_in_dim(query_nope, row_start, row_count, 0).reshape(row_count, HEADS, NOPE)
        turned = lax.dynamic_slice_in_dim(turned_query, row_start, row_count, 0)
        scores = jnp.einsum('qhd,khd->hqk', queries.astype(jnp.float32), key_rows.astype(jnp.float32))
        scores = scores + jnp.einsum('qhr,kr->hqk', turned.astype(jnp.float32), win_key.astype(jnp.float32))
        scores = jnp.where(allowed[None], scores * scale, masked_score)
        row_max = lax.optimization_barrier(jnp.max(scores, -1, keepdims=True))
        weights = jnp.exp(scores - row_max)
        weights = (weights / lax.optimization_barrier(jnp.sum(weights, -1, keepdims=True))).astype(jnp.bfloat16)
        attended = jnp.einsum('hqk,khd->qhd', weights.astype(jnp.float32), values.astype(jnp.float32)).astype(jnp.bfloat16).reshape(row_count, HEADS * VDIM)
        projected = jnp.zeros((row_count, D), jnp.float32)
        for member in range(N_TP):
            partial_value = jnp.dot(attended[:, member * head_group:(member + 1) * head_group], out_proj[member * head_group:(member + 1) * head_group], preferred_element_type=jnp.float32).astype(jnp.bfloat16)
            projected = projected + lax.optimization_barrier(partial_value).astype(jnp.float32)
        mixed = residual_scale * lax.dynamic_slice_in_dim(residual, row_start, row_count, 0).astype(jnp.float32) + projected
        return layer_norm(mixed, norm1_gain, norm1_bias).astype(jnp.bfloat16)
    normed = lax.map(first_half, jnp.arange(N_SP, dtype=jnp.int32)).reshape(TOKENS, D)
    padded_normed = jnp.concatenate([jnp.zeros((rim_rows, D), jnp.bfloat16), normed], 0)
    padded_doc_two = jnp.concatenate([jnp.full((rim_rows,), -1, jnp.int32), doc_ids], 0)
    unit_group = FF // N_TP

    def second_half(block_index):
        row_start = (block_index * row_count).astype(jnp.int32)
        own_pos = row_start + jnp.arange(row_count, dtype=jnp.int32)
        block_rows = lax.dynamic_slice_in_dim(padded_normed, row_start, row_count + rim_rows, 0)
        block_doc = lax.dynamic_slice_in_dim(padded_doc_two, row_start, row_count + rim_rows, 0)
        own_doc = block_doc[rim_rows:]
        gate_pre = jnp.dot(block_rows, ffn_gate, preferred_element_type=jnp.float32).astype(jnp.bfloat16)
        value_pre = jnp.dot(block_rows, ffn_value, preferred_element_type=jnp.float32).astype(jnp.bfloat16)
        gate_mix = jnp.zeros((row_count, FF), jnp.float32)
        value_mix = jnp.zeros((row_count, FF), jnp.float32)
        for tap_index in range(CONV):
            valid_tap = ((block_doc[tap_index:tap_index + row_count] == own_doc) & (own_pos - rim_rows + tap_index >= 0)).astype(jnp.float32)[:, None]
            gate_mix = gate_mix + conv_gate[tap_index].astype(jnp.float32) * gate_pre[tap_index:tap_index + row_count].astype(jnp.float32) * valid_tap
            value_mix = value_mix + conv_value[tap_index].astype(jnp.float32) * value_pre[tap_index:tap_index + row_count].astype(jnp.float32) * valid_tap
        hidden = (value_mix * jax.nn.gelu(gate_mix)).astype(jnp.bfloat16)
        ffn_out = jnp.zeros((row_count, D), jnp.float32)
        for member in range(N_TP):
            partial_value = jnp.dot(hidden[:, member * unit_group:(member + 1) * unit_group], ffn_down[member * unit_group:(member + 1) * unit_group], preferred_element_type=jnp.float32).astype(jnp.bfloat16)
            ffn_out = ffn_out + lax.optimization_barrier(partial_value).astype(jnp.float32)
        mixed = residual_scale * block_rows[rim_rows:].astype(jnp.float32) + ffn_out
        return layer_norm(mixed, norm2_gain, norm2_bias).astype(jnp.bfloat16)
    return lax.map(second_half, jnp.arange(N_SP, dtype=jnp.int32)).reshape(TOKENS, D)
```

```python
import jax
import jax.numpy as jnp
from jax import lax
from jax.sharding import PartitionSpec as P

D = 2048
NOPE = 128
ROPE = 64
VDIM = 128
CONV = 3
REACH = 3


norm_eps = 1e-05
residual_scale = 8.0**0.25
rope_base_freq = 10000.0
masked_score = -1e30


def passed_along(value, axis, by):
    count = lax.axis_size(axis)
    pairs = [(i, i + by) for i in range(count) if 0 <= i + by < count]
    return lax.ppermute(value, axis, pairs)


def tables(positions):
    frequencies = 1.0 / rope_base_freq ** (jnp.arange(0, ROPE, 2, dtype=jnp.float32) / ROPE)
    angles = positions.astype(jnp.float32)[:, None] * frequencies[None, :]
    return (jnp.cos(angles), jnp.sin(angles))


def rotate(vectors, cosine, sine_table):
    half_width = vectors.shape[-1] // 2
    front_half = vectors[..., :half_width]
    back_half = vectors[..., half_width:]
    return jnp.concatenate(
        [
            front_half * cosine - back_half * sine_table,
            front_half * sine_table + back_half * cosine,
        ],
        axis=-1,
    )


def scatter_sum(terms, axis):
    count = lax.axis_size(axis)
    width = terms.shape[1] // count
    parts = jnp.stack([terms[:, i * width : (i + 1) * width] for i in range(count)])
    got = lax.all_to_all(parts.astype(jnp.bfloat16), axis, 0, 0)
    return jnp.sum(got.astype(jnp.float32), 0)


def finish(mixed, totals, gain_row, bias_row):
    row_mean = totals[0][:, None] / D
    row_power = totals[1][:, None] / D
    return (mixed - row_mean) * lax.rsqrt(
        row_power - row_mean * row_mean + norm_eps
    ) * gain_row.astype(jnp.float32) + bias_row.astype(jnp.float32)


def local(
    residual,
    query_nope,
    query_rope,
    latent,
    rope_key,
    doc_ids,
    key_up,
    value_up,
    out_proj,
    norm1_gain,
    norm1_bias,
    ffn_gate,
    ffn_value,
    conv_gate,
    conv_value,
    ffn_down,
    norm2_gain,
    norm2_bias,
):
    row_count = latent.shape[0]
    head_count = query_nope.shape[1] // NOPE
    local_units = ffn_gate.shape[1]
    rim_rows = CONV - 1
    whole_gate, whole_value, whole_down = (
        lax.all_gather(ffn_gate, "sp", axis=0, tiled=True),
        lax.all_gather(ffn_value, "sp", axis=0, tiled=True),
        lax.all_gather(ffn_down, "sp", axis=1, tiled=True),
    )
    offset = lax.axis_index("sp") * row_count
    positions = offset + jnp.arange(row_count, dtype=jnp.int32)
    cosine, sine_table = tables(positions)
    turned_key = rotate(rope_key.astype(jnp.float32), cosine, sine_table).astype(jnp.bfloat16)
    turned_query = rotate(
        query_rope.astype(jnp.float32).reshape(row_count, head_count, ROPE),
        cosine[:, None],
        sine_table[:, None],
    ).astype(jnp.bfloat16)
    latent_list = []
    rim_list = []
    doc_list = []
    for shift_step in range(REACH, 0, -1):
        far_latent, far_key, far_doc = passed_along((latent, turned_key, doc_ids), "sp", shift_step)
        latent_list.append(far_latent)
        rim_list.append(far_key)
        doc_list.append(far_doc)
    win_latent = jnp.concatenate(latent_list + [latent], 0)
    win_key = jnp.concatenate(rim_list + [turned_key], 0)
    win_doc = jnp.concatenate(doc_list + [doc_ids], 0)
    key_rows = jnp.dot(win_latent, key_up, preferred_element_type=jnp.float32).astype(jnp.bfloat16)
    values = jnp.dot(win_latent, value_up, preferred_element_type=jnp.float32).astype(jnp.bfloat16)
    window = key_rows.shape[0]
    key_pos = offset - REACH * row_count + jnp.arange(window, dtype=jnp.int32)
    allowed = (
        (key_pos[None, :] <= positions[:, None])
        & (key_pos[None, :] >= 0)
        & (win_doc[None, :] == doc_ids[:, None])
    )
    scale = (NOPE + ROPE) ** (-0.5)
    scores = jnp.einsum(
        "qhd,khd->hqk",
        query_nope.reshape(row_count, head_count, NOPE),
        key_rows.reshape(window, head_count, NOPE),
        preferred_element_type=jnp.float32,
    )
    scores = scores + jnp.einsum(
        "qhr,kr->hqk", turned_query, win_key, preferred_element_type=jnp.float32
    )
    scores = jnp.where(allowed[None], scores * scale, masked_score)
    row_max = jnp.max(scores, -1, keepdims=True)
    weights = jnp.exp(scores - row_max)
    weights = (weights / jnp.sum(weights, -1, keepdims=True)).astype(jnp.bfloat16)
    attended = jnp.einsum(
        "hqk,khd->qhd",
        weights,
        values.reshape(window, head_count, VDIM),
        preferred_element_type=jnp.float32,
    )
    attended = attended.astype(jnp.bfloat16).reshape(row_count, head_count * VDIM)
    head_terms = jnp.dot(attended, out_proj, preferred_element_type=jnp.float32)
    projected = scatter_sum(head_terms, "tp")
    mixed_one = residual_scale * residual.astype(jnp.float32) + projected
    totals_one = lax.psum((jnp.sum(mixed_one, 1), jnp.sum(mixed_one * mixed_one, 1)), "tp")
    normed = finish(mixed_one, totals_one, norm1_gain, norm1_bias).astype(jnp.bfloat16)
    half = row_count // 2
    full_rows = jnp.concatenate(
        [
            lax.all_gather(normed[:half], "tp", axis=1, tiled=True),
            lax.all_gather(normed[half:], "tp", axis=1, tiled=True),
        ],
        0,
    )
    gate_sum = jnp.dot(full_rows, whole_gate, preferred_element_type=jnp.float32)
    value_sum = jnp.dot(full_rows, whole_value, preferred_element_type=jnp.float32)
    gate_pre = gate_sum.astype(jnp.bfloat16)
    value_pre = value_sum.astype(jnp.bfloat16)
    tail_gate, tail_value, tail_doc = passed_along(
        (
            gate_pre[row_count - rim_rows :],
            value_pre[row_count - rim_rows :],
            doc_ids[row_count - rim_rows :],
        ),
        "sp",
        1,
    )
    ext_gate = jnp.concatenate([tail_gate, gate_pre], 0)
    ext_value = jnp.concatenate([tail_value, value_pre], 0)
    ext_doc = jnp.concatenate([tail_doc, doc_ids], 0)
    gate_mix = jnp.zeros((row_count, local_units), jnp.float32)
    value_mix = jnp.zeros((row_count, local_units), jnp.float32)
    for tap_index in range(CONV):
        valid_tap = (
            (ext_doc[tap_index : tap_index + row_count] == doc_ids)
            & (positions - rim_rows + tap_index >= 0)
        ).astype(jnp.float32)[:, None]
        gate_mix = (
            gate_mix
            + conv_gate[tap_index].astype(jnp.float32)
            * ext_gate[tap_index : tap_index + row_count].astype(jnp.float32)
            * valid_tap
        )
        value_mix = (
            value_mix
            + conv_value[tap_index].astype(jnp.float32)
            * ext_value[tap_index : tap_index + row_count].astype(jnp.float32)
            * valid_tap
        )
    hidden = (value_mix * jax.nn.gelu(gate_mix)).astype(jnp.bfloat16)
    unit_terms = jnp.dot(hidden, whole_down, preferred_element_type=jnp.float32)
    ffn_out = scatter_sum(unit_terms, "tp")
    mixed_two = residual_scale * normed.astype(jnp.float32) + ffn_out
    totals_two = lax.psum((jnp.sum(mixed_two, 1), jnp.sum(mixed_two * mixed_two, 1)), "tp")
    return finish(mixed_two, totals_two, norm2_gain, norm2_bias).astype(jnp.bfloat16)


def solution(mesh):
    placed = (
        P("sp", "tp"),
        P("sp", "tp"),
        P("sp", "tp"),
        P("sp", None),
        P("sp", None),
        P("sp"),
        P(None, "tp"),
        P(None, "tp"),
        P("tp", None),
        P("tp"),
        P("tp"),
        P("sp", "tp"),
        P("sp", "tp"),
        P(None, "tp"),
        P(None, "tp"),
        P("tp", "sp"),
        P("tp"),
        P("tp"),
    )
    return jax.shard_map(
        local, mesh=mesh, in_specs=placed, out_specs=P("sp", "tp"), check_vma=False
    )
```

```python
import functools

import jax
import jax.numpy as jnp
from jax import lax
from jax.experimental import pallas as pl
from jax.experimental.pallas import tpu as pltpu
from jax.sharding import PartitionSpec as P

D = 2048
NOPE = 128
ROPE = 64
VDIM = 128
CONV = 3
REACH = 3


norm_eps = 1e-05
residual_scale = 8.0**0.25
rope_base_freq = 10000.0
masked_score = -1e30


def passed_along(value, axis, by):
    count = lax.axis_size(axis)
    pairs = [(i, i + by) for i in range(count) if 0 <= i + by < count]
    return lax.ppermute(value, axis, pairs)


def tables(positions):
    frequencies = 1.0 / rope_base_freq ** (jnp.arange(0, ROPE, 2, dtype=jnp.float32) / ROPE)
    angles = positions.astype(jnp.float32)[:, None] * frequencies[None, :]
    return (jnp.cos(angles), jnp.sin(angles))


def rotate(vectors, cosine, sine_table):
    half_width = vectors.shape[-1] // 2
    front_half = vectors[..., :half_width]
    back_half = vectors[..., half_width:]
    return jnp.concatenate(
        [
            front_half * cosine - back_half * sine_table,
            front_half * sine_table + back_half * cosine,
        ],
        axis=-1,
    )


def ring_blocks(block, axis):
    count = lax.axis_size(axis)
    order = list(range(0, count, 2)) + list(range(1, count, 2))[::-1]
    place = [order.index(i) for i in range(count)]
    me = lax.axis_index(axis)
    found = [(me, block)]
    ahead = count // 2
    for turn, steps in ((1, ahead), (-1, count - 1 - ahead)):
        pairs = [(order[p], order[(p + turn) % count]) for p in range(count)]
        moving = block
        for step in range(1, steps + 1):
            moving = lax.ppermute(moving, axis, pairs)
            owners = [order[(place[i] - turn * step) % count] for i in range(count)]
            found.append((jnp.asarray(owners, jnp.int32)[me], moving))
    return found


def attend_kernel(chunk, reach_rows, scale, q_ref, turned_ref, k_ref, rope_ref, v_ref, bias_ref, out_ref):
    rows = q_ref.shape[0]
    span = chunk + reach_rows
    rope_rows = rope_ref[...]
    for head in range(q_ref.shape[1] // NOPE):
        nope = slice(head * NOPE, (head + 1) * NOPE)
        rope = slice(head * ROPE, (head + 1) * ROPE)
        queries = jnp.concatenate([q_ref[:, nope], turned_ref[:, rope]], 1)
        keys = jnp.concatenate([k_ref[:, nope], rope_rows], 1)
        for start in range(0, rows, chunk):
            cut = slice(start, start + chunk)
            seen = slice(start, start + span)
            scores = lax.dot_general(
                queries[cut], keys[seen], (((1,), (1,)), ((), ())), preferred_element_type=jnp.float32
            )
            scores = scores * scale + bias_ref[cut, seen]
            weights = jnp.exp(scores - jnp.max(scores, -1, keepdims=True))
            weights = weights * (1.0 / jnp.sum(weights, -1, keepdims=True))
            out_ref[cut, nope] = jnp.dot(
                weights.astype(jnp.bfloat16), v_ref[seen, nope], preferred_element_type=jnp.float32
            ).astype(jnp.bfloat16)


def attend(queries, turned, keys, rope_rows, values, bias, scale):
    rows, width = queries.shape
    window = keys.shape[0]
    chunk = 128 if rows % 128 == 0 else rows
    pair = 2
    wide = pair * NOPE
    heads = width // NOPE
    return pl.pallas_call(
        functools.partial(attend_kernel, chunk, window - rows, scale),
        grid=(heads // pair,),
        in_specs=[
            pl.BlockSpec((rows, wide), lambda i: (0, i)),
            pl.BlockSpec((rows, pair * ROPE), lambda i: (0, i)),
            pl.BlockSpec((window, wide), lambda i: (0, i)),
            pl.BlockSpec((window, ROPE), lambda i: (0, 0)),
            pl.BlockSpec((window, pair * VDIM), lambda i: (0, i)),
            pl.BlockSpec((rows, window), lambda i: (0, 0)),
        ],
        out_specs=pl.BlockSpec((rows, pair * VDIM), lambda i: (0, i)),
        out_shape=jax.ShapeDtypeStruct((rows, heads * VDIM), jnp.bfloat16),
        compiler_params=pltpu.CompilerParams(vmem_limit_bytes=40 * 1024 * 1024),
        cost_estimate=pl.CostEstimate(
            flops=16 * rows * window * heads * (NOPE + ROPE + VDIM),
            bytes_accessed=2 * (4 * rows * width + 2 * window * width),
            transcendentals=rows * window * heads,
        ),
    )(queries, turned, keys, rope_rows, values, bias)


def scatter_sum(terms, axis):
    count = lax.axis_size(axis)
    width = terms.shape[1] // count
    parts = jnp.stack([terms[:, i * width : (i + 1) * width] for i in range(count)])
    got = lax.all_to_all(parts.astype(jnp.bfloat16), axis, 0, 0)
    return jnp.sum(got.astype(jnp.float32), 0)


def finish(mixed, totals, gain_row, bias_row):
    row_mean = totals[0][:, None] / D
    row_power = totals[1][:, None] / D
    return (mixed - row_mean) * lax.rsqrt(
        row_power - row_mean * row_mean + norm_eps
    ) * gain_row.astype(jnp.float32) + bias_row.astype(jnp.float32)


def local(
    residual,
    query_nope,
    query_rope,
    latent,
    rope_key,
    doc_ids,
    key_up,
    value_up,
    out_proj,
    norm1_gain,
    norm1_bias,
    ffn_gate,
    ffn_value,
    conv_gate,
    conv_value,
    ffn_down,
    norm2_gain,
    norm2_bias,
):
    row_count = latent.shape[0]
    head_count = query_nope.shape[1] // NOPE
    local_units = ffn_gate.shape[1]
    rim_rows = CONV - 1
    whole_gate = lax.all_gather(ffn_gate, "sp", axis=0, tiled=True)
    whole_value = lax.all_gather(ffn_value, "sp", axis=0, tiled=True)
    offset = lax.axis_index("sp") * row_count
    positions = offset + jnp.arange(row_count, dtype=jnp.int32)
    cosine, sine_table = tables(positions)
    turned_key = rotate(rope_key.astype(jnp.float32), cosine, sine_table).astype(jnp.bfloat16)
    turned_query = rotate(
        query_rope.astype(jnp.float32).reshape(row_count, head_count, ROPE),
        cosine[:, None],
        sine_table[:, None],
    ).astype(jnp.bfloat16)
    latent_width = latent.shape[1]
    packed = jnp.concatenate(
        [
            latent,
            turned_key,
            jnp.broadcast_to(doc_ids.astype(jnp.bfloat16)[:, None], (row_count, ROPE)),
        ],
        1,
    )
    parts = [passed_along(packed, "sp", shift_step) for shift_step in range(REACH, 0, -1)]
    pieces = jnp.concatenate(parts + [packed], 0)
    win_latent = pieces[:, :latent_width]
    win_key = pieces[:, latent_width : latent_width + ROPE]
    win_doc = pieces[:, latent_width + ROPE].astype(jnp.int32)
    down_blocks = ring_blocks(ffn_down, "sp")
    key_rows = jnp.dot(win_latent, key_up, preferred_element_type=jnp.float32).astype(jnp.bfloat16)
    values = jnp.dot(win_latent, value_up, preferred_element_type=jnp.float32).astype(jnp.bfloat16)
    window = key_rows.shape[0]
    key_pos = offset - REACH * row_count + jnp.arange(window, dtype=jnp.int32)
    allowed = (
        (key_pos[None, :] <= positions[:, None])
        & (key_pos[None, :] >= 0)
        & (win_doc[None, :] == doc_ids[:, None])
    )
    scale = (NOPE + ROPE) ** (-0.5)
    bias = jnp.where(allowed, 0.0, masked_score).astype(jnp.float32)
    attended = attend(
        query_nope,
        turned_query.reshape(row_count, head_count * ROPE),
        key_rows,
        win_key,
        values,
        bias,
        scale,
    )
    head_terms = jnp.dot(attended, out_proj, preferred_element_type=jnp.float32)
    projected = scatter_sum(head_terms, "tp")
    mixed_one = residual_scale * residual.astype(jnp.float32) + projected
    totals_one = lax.psum((jnp.sum(mixed_one, 1), jnp.sum(mixed_one * mixed_one, 1)), "tp")
    normed = finish(mixed_one, totals_one, norm1_gain, norm1_bias).astype(jnp.bfloat16)
    half = row_count // 2
    full_rows = jnp.concatenate(
        [
            lax.all_gather(normed[:half], "tp", axis=1, tiled=True),
            lax.all_gather(normed[half:], "tp", axis=1, tiled=True),
        ],
        0,
    )
    gate_sum = jnp.dot(full_rows, whole_gate, preferred_element_type=jnp.float32)
    value_sum = jnp.dot(full_rows, whole_value, preferred_element_type=jnp.float32)
    gate_pre = gate_sum.astype(jnp.bfloat16)
    value_pre = value_sum.astype(jnp.bfloat16)
    tail_gate, tail_value, tail_doc = passed_along(
        (
            gate_pre[row_count - rim_rows :],
            value_pre[row_count - rim_rows :],
            doc_ids[row_count - rim_rows :],
        ),
        "sp",
        1,
    )
    ext_gate = jnp.concatenate([tail_gate, gate_pre], 0)
    ext_value = jnp.concatenate([tail_value, value_pre], 0)
    ext_doc = jnp.concatenate([tail_doc, doc_ids], 0)
    gate_mix = jnp.zeros((row_count, local_units), jnp.float32)
    value_mix = jnp.zeros((row_count, local_units), jnp.float32)
    for tap_index in range(CONV):
        valid_tap = (
            (ext_doc[tap_index : tap_index + row_count] == doc_ids)
            & (positions - rim_rows + tap_index >= 0)
        ).astype(jnp.float32)[:, None]
        gate_mix = (
            gate_mix
            + conv_gate[tap_index].astype(jnp.float32)
            * ext_gate[tap_index : tap_index + row_count].astype(jnp.float32)
            * valid_tap
        )
        value_mix = (
            value_mix
            + conv_value[tap_index].astype(jnp.float32)
            * ext_value[tap_index : tap_index + row_count].astype(jnp.float32)
            * valid_tap
        )
    hidden = (value_mix * jax.nn.gelu(gate_mix)).astype(jnp.bfloat16)
    sp_count = lax.axis_size("sp")
    tp_count = lax.axis_size("tp")
    block_width = ffn_down.shape[1]
    unit_terms = jnp.zeros((sp_count, row_count, block_width), jnp.bfloat16)
    for owner, block in down_blocks:
        term = jnp.dot(hidden, block, preferred_element_type=jnp.float32).astype(jnp.bfloat16)
        unit_terms = lax.dynamic_update_slice(unit_terms, term[None], (owner, 0, 0))
    share = sp_count // tp_count
    got = lax.all_to_all(
        unit_terms.reshape(tp_count, share, row_count, block_width), "tp", 0, 0
    )
    ffn_blocks = jnp.sum(got.astype(jnp.float32), 0)
    ffn_out = jnp.concatenate([ffn_blocks[i] for i in range(share)], 1)
    mixed_two = residual_scale * normed.astype(jnp.float32) + ffn_out
    totals_two = lax.psum((jnp.sum(mixed_two, 1), jnp.sum(mixed_two * mixed_two, 1)), "tp")
    return finish(mixed_two, totals_two, norm2_gain, norm2_bias).astype(jnp.bfloat16)


def solution(mesh):
    placed = (
        P("sp", "tp"),
        P("sp", "tp"),
        P("sp", "tp"),
        P("sp", None),
        P("sp", None),
        P("sp"),
        P(None, "tp"),
        P(None, "tp"),
        P("tp", None),
        P("tp"),
        P("tp"),
        P("sp", "tp"),
        P("sp", "tp"),
        P(None, "tp"),
        P(None, "tp"),
        P("tp", "sp"),
        P("tp"),
        P("tp"),
    )
    return jax.shard_map(
        local, mesh=mesh, in_specs=placed, out_specs=P("sp", "tp"), check_vma=False
    )
```
